256 devices in a mesh: sp: 64 (over z, y, core), tp: 4 (over x).
Axes of the slice: x: 4, y: 4, z: 8, core: 2. Of those that a mesh axis runs over, the one named last changes fastest.
Arguments:
- tokens: bfloat16 [65536, 2048], P('sp'), may hold values from -6 to 6
- norm_gain: float32 [2048], replicated, may hold values from 0.1 to 1.9
- w_query: bfloat16 [2048, 1024], P('sp', 'tp'), may hold values from -3.5 to 3.5
- w_key: bfloat16 [2048, 256], P('sp', 'tp'), may hold values from -0.125 to 0.125
- w_value: bfloat16 [2048, 256], P('sp', 'tp'), may hold values from -0.125 to 0.125
- w_content: bfloat16 [2048, 1024], P('sp', 'tp'), may hold values from -0.125 to 0.125
- w_gate: bfloat16 [2048, 1024], P('sp', 'tp'), may hold values from -0.125 to 0.125
- sink_logit: float32 [16], P('tp'), may hold values from 1 to 6
- conv_weight: float32 [31, 1024], P(None, 'tp'), may hold values from -10 to 10
- conv_bias: float32 [1024], P('tp'), may hold values from 0 to 20
- channel_gain: float32 [1024], P('tp'), may hold values from 0.1 to 1.9
- out_attn: bfloat16 [1024, 2048], P('tp', 'sp'), may hold values from -0.75 to 0.75
- out_conv: bfloat16 [1024, 2048], P('tp', 'sp'), may hold values from -0.1875 to 0.1875
Outputs:
- mixed: bfloat16 [65536, 2048], P(('sp', 'tp'))
The draws below stay inside these ranges and needn't reach their ends.
All inputs are finite; a program needn't handle non-finite values.
Results may differ from the reference program's by a relative error of at most 0.025.
The reference program's roundings to bfloat16 on the way count: a program that leaves them out, or rounds other values in their place, can miss the bound.
Values may be sent and summed in bfloat16 or wider, within the bound.
No kernel may reach another device: no remote copies, remote signals or barrier semaphores. Data moves between devices by JAX's collectives and lax.ppermute only.
A program may use at most 64 MiB of HBM per device.

```python
import math
import jax
import jax.numpy as jnp
from jax import lax

D = 2048
HEADS = 16
KV_HEADS = 4
HEAD_DIM = 64
CONV_CH = 1024
KERNEL = 31
WINDOW = 128
TOKENS = 65536
ATTN_W = 1024
N_TP = 4


def draw_w_query(key, part):
    normal_part = jax.random.normal(key, (D, HEADS * HEAD_DIM), jnp.float32)
    return jnp.clip(normal_part / math.sqrt(D), -3.5, 3.5).astype(jnp.bfloat16)


def draw_conv_weight(key, part):
    normal_key = jax.random.fold_in(key, 11)
    jitter_key = jax.random.fold_in(key, 12)
    normal_part = jnp.clip(jax.random.normal(normal_key, (KERNEL, CONV_CH), jnp.float32), -4.0, 4.0)
    channel_ramp = jnp.arange(CONV_CH, dtype=jnp.float32) / CONV_CH
    jitter = jax.random.uniform(jitter_key, (CONV_CH,), jnp.float32, -0.3, 0.3)
    column_scale = 10.0 ** channel_ramp * jnp.exp(jitter) / math.sqrt(KERNEL)
    return normal_part * column_scale[None, :]


def draw_conv_bias(key, part):
    jitter_key = jax.random.fold_in(key, 21)
    channel_ramp = jnp.arange(CONV_CH, dtype=jnp.float32) / CONV_CH
    jitter = jax.random.uniform(jitter_key, (CONV_CH,), jnp.float32, 0.5, 1.5)
    return (0.5 + 9.5 * channel_ramp) * jitter


def levels(rng, dims, split, low, largest):
    def one(dim, blocks):
        steps = jax.random.uniform(jax.random.fold_in(jax.random.fold_in(rng, 6), dim), (blocks,), jnp.float32, low / len(split), largest / len(split))
        return jnp.repeat(jnp.exp(steps), dims[dim] // blocks).reshape((-1,) + (1,) * (len(dims) - dim - 1))

    factor_of = one(*split[0])
    for cut in split[1:]:
        factor_of = factor_of * one(*cut)
    return factor_of


def gaussian(key, extent, scale, limit, split=(), held_as=jnp.bfloat16):
    gain = levels(key, extent, split, -0.22, 0.18) if split else 1.0
    drawn = jax.random.normal(key, extent, jnp.float32) * scale * gain
    return jnp.minimum(jnp.maximum(drawn, -limit), limit).astype(held_as)


def setup_inputs(seed: int = 0) -> dict:
    key_of = jax.random.split(jax.random.key(seed), 14)
    tokens = gaussian(key_of[0], (TOKENS, D), 1.0, 6.0, ((0, 64),))
    norm_gain = jnp.clip(1.0 + 0.18 * jax.random.normal(key_of[1], (D,), jnp.float32), 0.1, 1.9)
    w_query = draw_w_query(jax.random.fold_in(key_of[13], 71), 0)
    w_key = gaussian(key_of[3], (D, KV_HEADS * HEAD_DIM), D ** -0.5, 0.125, ((0, 64), (1, 4)))
    w_value = gaussian(key_of[4], (D, KV_HEADS * HEAD_DIM), D ** -0.5, 0.125, ((0, 64), (1, 4)))
    w_content = gaussian(key_of[5], (D, CONV_CH), D ** -0.5, 0.125, ((0, 64), (1, 4)))
    w_gate = gaussian(key_of[6], (D, CONV_CH), D ** -0.5, 0.125, ((0, 64), (1, 4)))
    sink_logit = jnp.clip(1.0 + 5.0 * jax.random.uniform(key_of[7], (HEADS,), jnp.float32) ** levels(key_of[7], (HEADS,), ((0, 4),), -0.2, 0.2), 1.0, 6.0)
    conv_weight = draw_conv_weight(jax.random.fold_in(key_of[13], 71), 0)
    conv_bias = draw_conv_bias(jax.random.fold_in(key_of[13], 71), 0)
    channel_gain = jnp.clip(1.0 + 0.18 * jax.random.normal(key_of[10], (CONV_CH,), jnp.float32), 0.1, 1.9)
    out_attn = gaussian(key_of[11], (ATTN_W, D), (ATTN_W // 16) ** -0.5, 0.75, ((0, 4), (1, 64)))
    out_conv = gaussian(key_of[12], (CONV_CH, D), CONV_CH ** -0.5, 0.1875, ((0, 4), (1, 64)))
    return {"tokens": tokens, "norm_gain": norm_gain, "w_query": w_query, "w_key": w_key, "w_value": w_value, "w_content": w_content, "w_gate": w_gate, "sink_logit": sink_logit, "conv_weight": conv_weight, "conv_bias": conv_bias, "channel_gain": channel_gain, "out_attn": out_attn, "out_conv": out_conv}


EPS = 1e-05
THETA = 10000.0

def rotate(heads_in, positions):
    half_dim = heads_in.shape[-1] // 2
    inverse = 1.0 / THETA ** (jnp.arange(half_dim, dtype=jnp.float32) * 2.0 / heads_in.shape[-1])
    angles = positions.astype(jnp.float32)[:, None] * inverse[None, :]
    cosine = jnp.cos(angles)[:, None, :]
    sine_part = jnp.sin(angles)[:, None, :]
    former = heads_in[..., :half_dim]
    latter = heads_in[..., half_dim:]
    return jnp.concatenate([former * cosine - latter * sine_part, latter * cosine + former * sine_part], axis=-1)

def reference(tokens, norm_gain, w_query, w_key, w_value, w_content, w_gate, sink_logit, conv_weight, conv_bias, channel_gain, out_attn, out_conv):
    token_count = tokens.shape[0]
    positions = jnp.arange(token_count, dtype=jnp.int32)
    tokens_wide = tokens.astype(jnp.float32)
    inv_rms = lax.rsqrt(lax.optimization_barrier(jnp.mean(tokens_wide * tokens_wide, axis=1, keepdims=True)) + EPS)
    scaled = (tokens_wide * norm_gain[None, :]).astype(jnp.bfloat16)

    def project(weight):
        return jnp.dot(scaled, weight, preferred_element_type=jnp.float32) * inv_rms
    queries = rotate(project(w_query).reshape(token_count, HEADS, HEAD_DIM), positions).astype(jnp.bfloat16)
    key_rows = rotate(project(w_key).reshape(token_count, KV_HEADS, HEAD_DIM), positions).astype(jnp.bfloat16)
    value_rows = project(w_value).astype(jnp.bfloat16).reshape(token_count, KV_HEADS, HEAD_DIM)
    glu_out = (project(w_content) * jax.nn.sigmoid(project(w_gate))).astype(jnp.bfloat16)
    group_size = HEADS // KV_HEADS
    block_rows = math.gcd(token_count, 512)
    key_pad = jnp.concatenate([jnp.zeros((WINDOW, KV_HEADS, HEAD_DIM), jnp.bfloat16), key_rows], 0)
    value_pad = jnp.concatenate([jnp.zeros((WINDOW, KV_HEADS, HEAD_DIM), jnp.bfloat16), value_rows], 0)
    sink_col = sink_logit.reshape(KV_HEADS, group_size)[:, :, None, None]

    def attend(block_start):
        query_blk = lax.dynamic_slice_in_dim(queries, block_start, block_rows, 0).astype(jnp.float32)
        query_blk = query_blk.reshape(block_rows, KV_HEADS, group_size, HEAD_DIM)
        key_blk = lax.dynamic_slice_in_dim(key_pad, block_start, block_rows + WINDOW, 0).astype(jnp.float32)
        value_blk = lax.dynamic_slice_in_dim(value_pad, block_start, block_rows + WINDOW, 0).astype(jnp.float32)
        scores = jnp.einsum('qkgd,jkd->kgqj', query_blk, key_blk) * HEAD_DIM ** (-0.5)
        query_pos = block_start + jnp.arange(block_rows, dtype=jnp.int32)
        key_pos = block_start - WINDOW + jnp.arange(block_rows + WINDOW, dtype=jnp.int32)
        distance = query_pos[:, None] - key_pos[None, :]
        allowed = (distance >= 0) & (distance < WINDOW) & (key_pos[None, :] >= 0)
        scores = jnp.where(allowed[None, None], scores, -1e+30)
        row_max = jnp.maximum(lax.optimization_barrier(jnp.max(scores, axis=-1, keepdims=True)), sink_col)
        weights = jnp.exp(scores - row_max)
        denominator = lax.optimization_barrier(jnp.sum(weights, axis=-1, keepdims=True)) + jnp.exp(sink_col - row_max)
        probability = (weights / denominator).astype(jnp.bfloat16)
        attended = jnp.einsum('kgqj,jkd->qkgd', probability.astype(jnp.float32), value_blk)
        return attended.reshape(block_rows, HEADS * HEAD_DIM).astype(jnp.bfloat16)
    starts = jnp.arange(0, token_count, block_rows, dtype=jnp.int32)
    attn_out = lax.map(attend, starts).reshape(token_count, HEADS * HEAD_DIM)
    padded = jnp.concatenate([jnp.zeros((KERNEL - 1, CONV_CH), jnp.bfloat16), glu_out], 0)
    conv_sum = jnp.zeros((token_count, CONV_CH), jnp.float32) + conv_bias[None, :]
    for tap_index in range(KERNEL):
        window_rows = lax.slice_in_dim(padded, tap_index, tap_index + token_count, axis=0)
        conv_sum = conv_sum + conv_weight[tap_index][None, :] * window_rows.astype(jnp.float32)
    centre = lax.optimization_barrier(jnp.mean(conv_sum, axis=1, keepdims=True))
    centred = conv_sum - centre
    variance = lax.optimization_barrier(jnp.mean(centred * centred, axis=1, keepdims=True))
    conv_out = jax.nn.silu(centred * lax.rsqrt(variance + EPS) * channel_gain[None, :]).astype(jnp.bfloat16)
    attn_share = HEADS * HEAD_DIM // N_TP
    conv_share = CONV_CH // N_TP
    result = jnp.zeros((token_count, D), jnp.float32)
    for member in range(N_TP):
        partial_sum = jnp.dot(attn_out[:, member * attn_share:(member + 1) * attn_share], out_attn[member * attn_share:(member + 1) * attn_share], preferred_element_type=jnp.float32)
        partial_sum = partial_sum + jnp.dot(conv_out[:, member * conv_share:(member + 1) * conv_share], out_conv[member * conv_share:(member + 1) * conv_share], preferred_element_type=jnp.float32)
        rounded = lax.optimization_barrier(partial_sum.astype(jnp.bfloat16))
        result = result + rounded.astype(jnp.float32)
    return result.astype(jnp.bfloat16)
```

```python
import functools

import jax
import jax.numpy as jnp
import numpy as np
from jax import lax
from jax.experimental import pallas as pl
from jax.experimental.pallas import tpu as pltpu
from jax.sharding import Mesh
from jax.sharding import PartitionSpec as P


HEAD_DIM = 64
CONV_CH = 1024
KERNEL = 31
WINDOW = 128
EPS = 1e-05
THETA = 10000.0
SP = ("z", "y", "c")
NX = 4
F32 = jnp.float32
BF16 = jnp.bfloat16
VMEM_LIMIT = 60 * 1024 * 1024


def to_partner(v, table):
    out = lax.ppermute(v, "c", [(0, 1), (1, 0)])
    return out, [(-a, -b, d ^ 1) for a, b, d in table]


def onward(v, table, axis):
    size = lax.axis_size(axis)
    route = []
    for i in range(size):
        route.append((i * 2, ((i + 1) % size) * 2))
        route.append((i * 2 + 1, ((i - 1) % size) * 2 + 1))
    out = lax.ppermute(v, (axis, "c"), route)
    if axis == "z":
        return out, [(a - 1, b, d) for a, b, d in table]
    return out, [(a, b - 1, d) for a, b, d in table]


def round_trip(v, table, axis):
    half = lax.axis_size(axis) // 2
    got = []
    for step in range(1, half + 1):
        if step == half:
            rows = v.shape[0] // 2
            v, table = v[:rows], table[: len(table) // 2]
        v, table = onward(v, table, axis)
        got.append((v, table))
    return got


def joined(parts):
    return jnp.concatenate([v for v, _ in parts], 0), sum((t for _, t in parts), [])


def gather_rows(v, axes):
    own = (v, [(0, 0, 0)])
    block = joined([own, to_partner(*own)])
    mine = joined([own] + round_trip(*block, axes[0]))
    block = joined([mine, to_partner(*mine)])
    got = round_trip(*block, axes[1])
    parts = [block]
    for part in got:
        parts += [part, to_partner(*part)]
    return parts


def places(parts):
    table = np.array(sum((t for _, t in parts), []), np.int32)
    z, y, c = (lax.axis_index(a) for a in SP)
    s = 1 - 2 * c
    return (((z + s * table[:, 0]) % 8) * 8 + ((y + s * table[:, 1]) % 4) * 2 + (c ^ table[:, 2])).astype(jnp.int32)


def around_x(blocks):
    out = [blocks[0]]
    for r in range(1, NX):
        out.append(lax.ppermute(blocks[r], "x", [(i, (i + r) % NX) for i in range(NX)]))
    return out


def vmem(n):
    return [pl.BlockSpec(memory_space=pltpu.VMEM)] * n


SMEM = pl.BlockSpec(memory_space=pltpu.SMEM)


def params():
    return pltpu.CompilerParams(vmem_limit_bytes=VMEM_LIMIT)


def put_rows(place_ref, piece_refs, w_ref):
    k = 0
    for ref in piece_refs:
        for row in range(0, ref.shape[0], 32):
            at = pl.multiple_of(place_ref[k] * 32, 32)
            w_ref[pl.ds(at, 32), :] = ref[row : row + 32, :]
            k += 1


def lane_is(shape, period, limit):
    return lax.broadcasted_iota(jnp.int32, shape, len(shape) - 1) % period < limit


def turn(x, cosine, sine):
    other = jnp.where(lane_is(x.shape, 64, 32), pltpu.roll(x, 96, 1), pltpu.roll(x, 32, 1))
    return x * cosine + other * sine


def qkv_kernel(n_pieces, place_ref, *refs):
    pieces = refs[:n_pieces]
    x_ref, inv_ref, cos_ref, sin_ref, q_ref, kv_ref, w_ref = refs[n_pieces:]
    put_rows(place_ref, pieces, w_ref)

    def tile(i, _):
        rows = pl.ds(pl.multiple_of(i * 256, 256), 256)
        out = jnp.dot(x_ref[rows, :], w_ref[...], preferred_element_type=F32) * inv_ref[rows, :]
        cosine, sine = cos_ref[rows, :], sin_ref[rows, :]
        for p in range(2):
            turned = turn(out[:, p * 128 : p * 128 + 128], cosine, sine).astype(BF16)
            q_ref[rows, p * 128 : p * 128 + 128] = turned * BF16(HEAD_DIM**-0.5)
        kv = out[:, 256:384]
        vk = pltpu.roll(kv, 64, 1)
        first = lane_is(kv.shape, 128, 64)
        kv_ref[rows, 0:128] = turn(jnp.where(first, kv, vk), cosine, sine).astype(BF16)
        kv_ref[rows, 128:256] = jnp.where(first, vk, kv).astype(BF16)
        return 0

    lax.fori_loop(0, x_ref.shape[0] // 256, tile, 0)


def glu_kernel(n_pieces, place_ref, *refs):
    pieces = refs[:n_pieces]
    x_ref, inv_ref, glu_ref, w_ref = refs[n_pieces:]
    put_rows(place_ref, pieces, w_ref)

    def tile(i, _):
        rows = pl.ds(pl.multiple_of(i * 256, 256), 256)
        out = jnp.dot(x_ref[rows, :], w_ref[...], preferred_element_type=F32) * inv_ref[rows, :]
        glu_ref[rows, :] = (out[:, :256] * jax.nn.sigmoid(out[:, 256:])).astype(BF16)
        return 0

    lax.fori_loop(0, x_ref.shape[0] // 256, tile, 0)


def attention_kernel(first_ref, sink_ref, q_ref, kv_ref, prior_ref, out_ref, k_ref, v_ref):
    tokens = q_ref.shape[0]
    for half in range(2):
        for src, dst, lane in ((prior_ref, 0, 0), (kv_ref, WINDOW, 0)):
            rows = src.shape[0]
            keep = lane_is((rows, 128), 128, 64)
            if half:
                keep = jnp.logical_not(keep)
            zero = jnp.zeros((rows, 128), BF16)
            k_ref[half, dst : dst + rows, :] = jnp.where(keep, src[:, 0:128], zero)
            v_ref[half, dst : dst + rows, :] = jnp.where(keep, src[:, 128:256], zero)
    row = lax.broadcasted_iota(jnp.int32, (128, 256), 0)
    col = lax.broadcasted_iota(jnp.int32, (128, 256), 1)
    band = (col > row) & (col <= row + 128)

    def block(b, _):
        at = pl.multiple_of(b * 128, 128)
        lowest = jnp.where(b == 0, first_ref[0], 0)
        allowed = band & (col >= lowest)
        for pair in range(2):
            q = q_ref[pl.ds(at, 128), pair * 128 : pair * 128 + 128]
            total = None
            for half in range(2):
                scores = lax.dot_general(
                    q, k_ref[half, pl.ds(at, 256), :], (((1,), (1,)), ((), ())), preferred_element_type=F32
                )
                scores = jnp.where(allowed, scores, -1e30)
                sink = sink_ref[pair * 2 + half]
                row_max = jnp.maximum(jnp.max(scores, axis=1, keepdims=True), sink)
                weights = jnp.exp(scores - row_max)
                denominator = jnp.sum(weights, axis=1, keepdims=True) + jnp.exp(sink - row_max)
                probability = (weights * (1.0 / denominator)).astype(BF16)
                part = jnp.dot(probability, v_ref[half, pl.ds(at, 256), :], preferred_element_type=F32)
                total = part if total is None else total + part
            out_ref[pl.ds(at, 128), pair * 128 : pair * 128 + 128] = total.astype(BF16)
        return 0

    lax.fori_loop(0, tokens // 128, block, 0, unroll=2)


def conv_kernel(glu_ref, prior_ref, w_ref, out_ref, shift_ref):
    tokens = glu_ref.shape[0]
    shift_ref[0, 0:32, :] = prior_ref[...].astype(F32)
    shift_ref[0, 32 : 32 + tokens, :] = glu_ref[...].astype(F32)

    def fill(i, _):
        at = pl.multiple_of(i * 32, 32)
        rows = shift_ref[0, pl.ds(at, 40), :]
        for b in range(1, 8):
            shift_ref[b, pl.ds(at, 32), :] = rows[b : b + 32, :]
        return 0

    lax.fori_loop(0, tokens // 32 + 1, fill, 0)

    def tile(i, _):
        at = pl.multiple_of(i * 32, 32)
        total = None
        for j in range(KERNEL):
            ahead, b = divmod(j + 2, 8)
            term = w_ref[j : j + 1, :] * shift_ref[b, pl.ds(at + ahead * 8, 32), :]
            total = term if total is None else total + term
        out_ref[pl.ds(at, 32), :] = total.astype(BF16)
        return 0

    lax.fori_loop(0, tokens // 32, tile, 0)


def out_kernel(n_pieces, place_ref, *refs):
    pieces = refs[:n_pieces]
    attn = refs[n_pieces : n_pieces + NX]
    conv = refs[n_pieces + NX : n_pieces + 2 * NX]
    edge = refs[n_pieces + 2 * NX : n_pieces + 3 * NX]
    out_ref, w_ref, act_ref = refs[n_pieces + 3 * NX :]
    put_rows(place_ref, pieces, w_ref)
    wide = attn[0].shape[1]
    for r in range(NX):
        act_ref[:, r * wide : (r + 1) * wide] = attn[r][...]
    sums = [conv[r][...].astype(F32) + edge[r][0:1, :] for r in range(NX)]
    centre = sum(jnp.sum(s, axis=1, keepdims=True) for s in sums) * (1.0 / CONV_CH)
    centred = [s - centre for s in sums]
    variance = sum(jnp.sum(s * s, axis=1, keepdims=True) for s in centred) * (1.0 / CONV_CH)
    scale = lax.rsqrt(variance + EPS)
    for r in range(NX):
        value = centred[r] * scale * edge[r][1:2, :]
        act_ref[:, (NX + r) * wide : (NX + r + 1) * wide] = (value * jax.nn.sigmoid(value)).astype(BF16)

    def tile(i, _):
        at = pl.multiple_of(i * 256, 256)
        out_ref[:, pl.ds(at, 256)] = lax.dot_general(
            act_ref[...], w_ref[pl.ds(at, 256), :], (((1,), (1,)), ((), ())), preferred_element_type=F32
        ).astype(BF16)
        return 0

    lax.fori_loop(0, out_ref.shape[1] // 256, tile, 0)


def cost(flops, moved):
    return pl.CostEstimate(flops=flops, bytes_accessed=moved, transcendentals=0)


def shards(
    tokens, norm_gain, w_query, w_key, w_value, w_content, w_gate, sink_logit,
    conv_weight, conv_bias, channel_gain, out_attn, out_conv,
):
    count = tokens.shape[0]
    sp_index = lax.axis_index(SP)
    x_index = lax.axis_index("x")

    qkv_parts = gather_rows(jnp.concatenate([w_query, w_key, w_value], 1), ("y", "z"))
    cg_parts = gather_rows(jnp.concatenate([w_content, w_gate], 1), ("y", "z"))
    place = places(qkv_parts)

    out_own = jnp.concatenate([out_attn.T, out_conv.T], 1)
    out_x = around_x([out_own] * NX)
    width = out_attn.shape[0]
    out_x = jnp.concatenate([o[:, :width] for o in out_x] + [o[:, width:] for o in out_x], 1)
    out_parts = gather_rows(out_x, ("y", "z"))
    place_out = places(out_parts)
    edge = around_x([jnp.stack([conv_bias, channel_gain])] * NX)

    wide = tokens.astype(F32)
    inv_rms = lax.rsqrt(jnp.mean(wide * wide, axis=1, keepdims=True) + EPS)
    scaled = (wide * norm_gain[None, :]).astype(BF16)

    half = HEAD_DIM // 2
    inverse = 1.0 / THETA ** (jnp.arange(half, dtype=F32) * 2.0 / HEAD_DIM)
    positions = sp_index * count + jnp.arange(count, dtype=jnp.int32)
    angles = positions.astype(F32)[:, None] * jnp.tile(inverse, 4)[None, :]
    cosine = jnp.cos(angles)
    sine = jnp.sin(angles) * jnp.asarray(np.repeat([-1.0, 1.0, -1.0, 1.0], half), F32)[None, :]

    pieces = [v for v, _ in qkv_parts]
    queries, keys_values = pl.pallas_call(
        functools.partial(qkv_kernel, len(pieces)),
        out_shape=(
            jax.ShapeDtypeStruct((count, 256), BF16),
            jax.ShapeDtypeStruct((count, 256), BF16),
        ),
        in_specs=[SMEM] + vmem(len(pieces) + 4),
        out_specs=tuple(vmem(2)),
        scratch_shapes=[pltpu.VMEM((2048, 384), BF16)],
        compiler_params=params(),
        cost_estimate=cost(2 * count * 2048 * 384, 8 << 20),
    )(place, *pieces, scaled, inv_rms, cosine, sine)

    ahead = [(i, i + 1) for i in range(63)]
    prior_kv = lax.ppermute(keys_values[count - WINDOW :], SP, ahead)

    pieces = [v for v, _ in cg_parts]
    glu = pl.pallas_call(
        functools.partial(glu_kernel, len(pieces)),
        out_shape=jax.ShapeDtypeStruct((count, 256), BF16),
        in_specs=[SMEM] + vmem(len(pieces) + 2),
        out_specs=vmem(1)[0],
        scratch_shapes=[pltpu.VMEM((2048, 512), BF16)],
        compiler_params=params(),
        cost_estimate=cost(2 * count * 2048 * 512, 8 << 20),
    )(place, *pieces, scaled, inv_rms)
    prior_glu = lax.ppermute(glu[count - 32 :], SP, ahead)

    first = jnp.where(sp_index == 0, WINDOW, 0).astype(jnp.int32).reshape(1)
    attended = pl.pallas_call(
        attention_kernel,
        out_shape=jax.ShapeDtypeStruct((count, 256), BF16),
        in_specs=[SMEM, SMEM] + vmem(3),
        out_specs=vmem(1)[0],
        scratch_shapes=[pltpu.VMEM((2, WINDOW + count, 128), BF16)] * 2,
        compiler_params=params(),
        cost_estimate=cost(2 * count * 2048 * 512, 8 << 20),
    )(first, sink_logit, queries, keys_values, prior_kv)

    def block_for(v, r):
        share = count // NX
        return lax.dynamic_slice_in_dim(v, ((x_index + r) % NX) * share, share, 0)

    attn_blocks = around_x([block_for(attended, r) for r in range(NX)])

    conv_sum = pl.pallas_call(
        conv_kernel,
        out_shape=jax.ShapeDtypeStruct((count, 256), BF16),
        in_specs=vmem(3),
        out_specs=vmem(1)[0],
        scratch_shapes=[pltpu.VMEM((8, count + 48, 256), F32)],
        compiler_params=params(),
        cost_estimate=cost(2 * count * 2048 * 512, 8 << 20),
    )(glu, prior_glu, conv_weight)
    conv_blocks = around_x([block_for(conv_sum, r) for r in range(NX)])

    pieces = [v for v, _ in out_parts]
    return pl.pallas_call(
        functools.partial(out_kernel, len(pieces)),
        out_shape=jax.ShapeDtypeStruct((count // NX, 2048), BF16),
        in_specs=[SMEM] + vmem(len(pieces) + 3 * NX),
        out_specs=vmem(1)[0],
        scratch_shapes=[pltpu.VMEM((2048, 2048), BF16), pltpu.VMEM((count // NX, 2048), BF16)],
        compiler_params=params(),
        cost_estimate=cost(2 * 256 * 2048 * 2048, 12 << 20),
    )(place_out, *pieces, *attn_blocks, *conv_blocks, *edge)


def solution(mesh):
    torus = Mesh(mesh.devices.reshape(8, 4, 2, mesh.shape["tp"]), ("z", "y", "c", "x"))
    return jax.shard_map(
        shards,
        mesh=torus,
        in_specs=(
            P(SP, None), P(), P(SP, "x"), P(SP, "x"), P(SP, "x"), P(SP, "x"), P(SP, "x"), P("x"),
            P(None, "x"), P("x"), P("x"), P("x", SP), P("x", SP),
        ),
        out_specs=P((*SP, "x"), None),
        check_vma=False,
    )
```

```python
import functools

import jax
import jax.numpy as jnp
import numpy as np
from jax import lax
from jax.experimental import pallas as pl
from jax.experimental.pallas import tpu as pltpu
from jax.sharding import Mesh
from jax.sharding import PartitionSpec as P


HEAD_DIM = 64
CONV_CH = 1024
KERNEL = 31
WINDOW = 128
EPS = 1e-05
THETA = 10000.0
SP = ("z", "y", "c")
NX = 4
F32 = jnp.float32
BF16 = jnp.bfloat16


OWN = [(0, 0, 0, 0, 0)]


def to_partner(v, table):
    out = lax.ppermute(v, "c", [(0, 1), (1, 0)])
    return out, [(-a, -b, d ^ 1, e, -f) for a, b, d, e, f in table]


def onward(v, table, axis):
    size = lax.axis_size(axis)
    route = []
    for i in range(size):
        up, down = (i + 1) % size, (i - 1) % size
        if axis == "x":
            route += [(i, up), (size + i, size + down)]
        else:
            route += [(i * 2, up * 2), (i * 2 + 1, down * 2 + 1)]
    out = lax.ppermute(v, ("c", "x") if axis == "x" else (axis, "c"), route)
    k = {"z": 0, "y": 1, "x": 4}[axis]
    return out, [t[:k] + (t[k] - 1,) + t[k + 1 :] for t in table]


def go_round(v, table, axis):
    got = []
    for _ in range(lax.axis_size(axis) // 2):
        v, table = onward(v, table, axis)
        got.append((v, table))
    return got


def copy_kernel(plan, n_in, *refs):
    sources, results = refs[:n_in], refs[n_in:]
    for out, row, lane, src, row_0, lane_0, rows, lanes in plan:
        results[out][row : row + rows, lane : lane + lanes] = sources[src][row_0 : row_0 + rows, lane_0 : lane_0 + lanes]


def copied(sources, plan, shapes):
    outs = kernel_call(
        functools.partial(copy_kernel, plan, len(sources)),
        out_shape=tuple(jax.ShapeDtypeStruct(shape, BF16) for shape in shapes),
        in_specs=vmem(len(sources)),
        out_specs=tuple(vmem(len(shapes))),
        compiler_params=params(4),
        cost_estimate=cost(1 << 20, 1 << 20),
    )(*sources)
    return list(outs)


def join(parts, lo=0, hi=None):
    hi = hi or parts[0][0].shape[1]
    plan, row = [], 0
    for k, (v, _) in enumerate(parts):
        plan.append((0, row, 0, k, 0, lo, v.shape[0], hi - lo))
        row += v.shape[0]
    out = copied([v for v, _ in parts], plan, [(row, hi - lo)])[0]
    return out, sum((t for _, t in parts), [])


def tables(parts):
    return tuple(tuple(t) for _, t in parts)


def shift(v, axis, r):
    size = lax.axis_size(axis)
    return lax.ppermute(v, axis, [(i, (i + r) % size) for i in range(size)])


def around_x(blocks):
    return [blocks[0]] + [shift(blocks[r], "x", r) for r in range(1, NX)]


def around_y(v, table):
    return [(v, table)] + [(shift(v, "y", r), [(a, b, d, e - r, f) for a, b, d, e, f in table]) for r in (1, 3, 2)]


def kernel_call(body, **keys):
    return pl.pallas_call(body, **keys)


def vmem(n):
    return [pl.BlockSpec(memory_space=pltpu.VMEM)] * n


SMEM = pl.BlockSpec(memory_space=pltpu.SMEM)


def params(mib):
    return pltpu.CompilerParams(vmem_limit_bytes=mib * 1024 * 1024)


def put_rows(table, piece_refs, w_ref, across=False):
    z, y, c = (lax.axis_index(a) for a in SP)
    s = 1 - 2 * c
    for ref, places in zip(piece_refs, table):
        width = min(w_ref.shape[1], ref.shape[1])
        lane = pl.multiple_of(((-s * places[0][4]) & 3) * width, 128) if across else 0
        for k, (a, b, d, e, _) in enumerate(places):
            block = ((z + s * a) & 7) * 8 + ((y + s * b + e) & 3) * 2 + (c ^ d)
            row = pl.multiple_of(block * 32, 32)
            w_ref[pl.ds(row, 32), pl.ds(lane, width)] = ref[32 * k : 32 * k + 32, 0:width]


def lane_is(shape, period, limit):
    return lax.broadcasted_iota(jnp.int32, shape, len(shape) - 1) % period < limit


def sp_place():
    return (lax.axis_index("z") * 4 + lax.axis_index("y")) * 2 + lax.axis_index("c")


def turn(x, cosine, sine):
    other = jnp.where(lane_is(x.shape, 64, 32), pltpu.roll(x, 96, 1), pltpu.roll(x, 32, 1))
    return x * cosine + other * sine


def prep_kernel(tokens_ref, prior_ref, gain_ref, scaled_ref, inv_ref):
    def scale(wide, i):
        rows = pl.ds(pl.multiple_of(i * 32, 32), 32)
        scaled_ref[rows, :] = (wide * gain_ref[...]).astype(BF16)
        mean = jnp.sum(wide * wide, axis=1, keepdims=True) * (1.0 / wide.shape[1])
        inv_ref[rows, :] = jnp.broadcast_to(lax.rsqrt(mean + EPS), (32, 128))

    def before(i, _):
        scale(prior_ref[pl.ds(pl.multiple_of(i * 32, 32), 32), :].astype(F32), i)
        return 0

    def tile(i, _):
        scale(tokens_ref[pl.ds(pl.multiple_of(i * 32, 32), 32), :].astype(F32), i + WINDOW // 32)
        return 0

    lax.fori_loop(0, WINDOW // 32, before, 0)
    lax.fori_loop(0, tokens_ref.shape[0] // 32, tile, 0, unroll=2)


def rope_tables():
    half = HEAD_DIM // 2
    inverse = np.tile(1.0 / THETA ** (np.arange(half) * 2.0 / HEAD_DIM), 4)[None, :]
    steps = np.concatenate([np.arange(32), 1024 * np.arange(64), 32 * np.arange(-4, 36)])[:, None]
    return jnp.asarray(np.cos(steps * inverse), F32), jnp.asarray(np.sin(steps * inverse), F32)


def times_inv(out, inv):
    return jnp.concatenate([out[:, k : k + 128] * inv for k in range(0, out.shape[1], 128)], 1)


def qkv_kernel(table, *refs):
    n_pieces = len(table)
    pieces = refs[:n_pieces]
    x_ref, inv_ref, cos_ref, sin_ref, q_ref, kv_ref, w_ref = refs[n_pieces:]
    put_rows(table, pieces, w_ref)
    sp = sp_place()
    size = 384

    def tile(i, _):
        rows = pl.ds(pl.multiple_of(i * size, 128), size)
        out = jnp.dot(x_ref[rows, :], w_ref[...], preferred_element_type=F32)
        out = times_inv(out, inv_ref[rows, :])
        ca, sa = cos_ref[pl.ds(32 + sp, 1), :], sin_ref[pl.ds(32 + sp, 1), :]
        cl, sl = cos_ref[0:32, :], sin_ref[0:32, :]
        cosines, sines = [], []
        for j in range(size // 32):
            at = pl.ds(96 + i * (size // 32) + j, 1)
            cb, sb = cos_ref[at, :], sin_ref[at, :]
            ch, sh = ca * cb - sa * sb, sa * cb + ca * sb
            cosines.append(ch * cl - sh * sl)
            sines.append(sh * cl + ch * sl)
        cosine, sine = jnp.concatenate(cosines, 0), jnp.concatenate(sines, 0)
        sine = jnp.where(lane_is(sine.shape, 64, 32), -sine, sine)
        for p in range(2):
            turned = turn(out[:, p * 128 : p * 128 + 128], cosine, sine).astype(BF16)
            q_ref[rows, p * 128 : p * 128 + 128] = turned * BF16(HEAD_DIM**-0.5)
        kv = out[:, 256:384]
        vk = pltpu.roll(kv, 64, 1)
        first = lane_is(kv.shape, 128, 64)
        kv_ref[rows, 0:128] = turn(jnp.where(first, kv, vk), cosine, sine).astype(BF16)
        kv_ref[rows, 128:256] = jnp.where(first, vk, kv).astype(BF16)
        return 0

    lax.fori_loop(0, x_ref.shape[0] // size, tile, 0)


def glu_kernel(table, *refs):
    n_pieces = len(table)
    pieces = refs[:n_pieces]
    x_ref, inv_ref, glu_ref, w_ref = refs[n_pieces:]
    put_rows(table, pieces, w_ref)
    size = 384

    def tile(i, _):
        rows = pl.ds(pl.multiple_of(i * size, 128), size)
        out = jnp.dot(x_ref[rows, :], w_ref[...], preferred_element_type=F32)
        out = times_inv(out, inv_ref[rows, :])
        glu_ref[rows, :] = (out[:, :256] * jax.nn.sigmoid(out[:, 256:])).astype(BF16)
        return 0

    lax.fori_loop(0, x_ref.shape[0] // size, tile, 0)


def attention_kernel(sink_ref, q_ref, kv_ref, *refs):
    block_refs, (k_ref, v_ref, out_ref) = refs[:NX], refs[NX:]
    tokens = q_ref.shape[0] - WINDOW
    for half in range(2):
        for src, dst in ((kv_ref, 0),):
            rows = src.shape[0]
            keep = lane_is((rows, 128), 128, 64)
            if half:
                keep = jnp.logical_not(keep)
            zero = jnp.zeros((rows, 128), BF16)
            k_ref[half, dst : dst + rows, :] = jnp.where(keep, src[:, 0:128], zero)
            v_ref[half, dst : dst + rows, :] = jnp.where(keep, src[:, 128:256], zero)
    row = lax.broadcasted_iota(jnp.int32, (128, 256), 0)
    col = lax.broadcasted_iota(jnp.int32, (128, 256), 1)
    band = (col > row) & (col <= row + 128)

    def block(b, _):
        at = pl.multiple_of(b * 128, 128)
        lowest = jnp.where((b == 0) & (sp_place() == 0), WINDOW, 0)
        allowed = band & (col >= lowest)
        for pair in range(2):
            q = q_ref[pl.ds(at + WINDOW, 128), pair * 128 : pair * 128 + 128]
            total = None
            for half in range(2):
                scores = lax.dot_general(
                    q, k_ref[half, pl.ds(at, 256), :], (((1,), (1,)), ((), ())), preferred_element_type=F32
                )
                scores = jnp.where(allowed, scores, -1e30)
                sink = sink_ref[pair * 2 + half]
                row_max = jnp.maximum(jnp.max(scores, axis=1, keepdims=True), sink)
                weights = jnp.exp(scores - row_max)
                denominator = jnp.sum(weights, axis=1, keepdims=True) + jnp.exp(sink - row_max)
                probability = (weights * (1.0 / denominator)).astype(BF16)
                part = jnp.dot(probability, v_ref[half, pl.ds(at, 256), :], preferred_element_type=F32)
                total = part if total is None else total + part
            out_ref[pl.ds(at, 128), pair * 128 : pair * 128 + 128] = total.astype(BF16)
        return 0

    lax.fori_loop(0, tokens // 128, block, 0, unroll=2)
    to_blocks(out_ref, block_refs)


def to_blocks(src_ref, block_refs):
    share = src_ref.shape[0] // NX
    for r, ref in enumerate(block_refs):
        at = pl.multiple_of(((lax.axis_index("x") + r) & 3) * share, share)
        ref[0:share, :] = src_ref[pl.ds(at, share), :]


def conv_kernel(glu_ref, w_ref, bias_ref, gain_ref, *refs):
    block_refs, (shift_ref, out_ref) = refs[:NX], refs[NX:]
    tokens = glu_ref.shape[0] - WINDOW
    shift_ref[0, 0 : 32 + tokens, :] = glu_ref[WINDOW - 32 :, :].astype(F32)

    def fill(i, _):
        at = pl.multiple_of(i * 32, 32)
        rows = shift_ref[0, pl.ds(at, 40), :]
        for b in range(1, 8):
            shift_ref[b, pl.ds(at, 32), :] = rows[b : b + 32, :]
        return 0

    lax.fori_loop(0, tokens // 32 + 1, fill, 0)

    def tile(i, _):
        at = pl.multiple_of(i * 32, 32)
        total = None
        for j in range(KERNEL):
            ahead, b = divmod(j + 2, 8)
            term = w_ref[j : j + 1, :] * shift_ref[b, pl.ds(at + ahead * 8, 32), :]
            total = term if total is None else total + term
        out_ref[pl.ds(at, 32), :] = total.astype(BF16)
        return 0

    lax.fori_loop(0, tokens // 32, tile, 0)
    to_blocks(out_ref, block_refs)
    edge = jnp.concatenate([bias_ref[...], gain_ref[...]], 0)
    high = edge.astype(BF16).astype(F32)
    middle = (edge - high).astype(BF16).astype(F32)
    low = edge - high - middle
    rows = jnp.concatenate([high, middle, low, jnp.zeros((16 - 3 * edge.shape[0], edge.shape[1]), F32)], 0).astype(BF16)
    for ref in block_refs:
        ref[ref.shape[0] - 16 :, :] = rows


def out_attn_kernel(table, *refs):
    n_pieces = len(table)
    pieces, refs = refs[:n_pieces], refs[n_pieces:]
    attn, (out_ref, w_ref, act_ref) = refs[:NX], refs[NX:]
    put_rows(table, pieces, w_ref)
    wide = attn[0].shape[1]
    for r in range(NX):
        act_ref[:, r * wide : (r + 1) * wide] = attn[r][...]

    def tile(i, _):
        at = pl.multiple_of(i * 256, 256)
        out_ref[:, pl.ds(at, 256)] = lax.dot_general(
            act_ref[...], w_ref[pl.ds(at, 256), :], (((1,), (1,)), ((), ())), preferred_element_type=F32
        )
        return 0

    lax.fori_loop(0, out_ref.shape[1] // 256, tile, 0)


def out_conv_kernel(table, *refs):
    n_pieces = len(table)
    pieces, refs = refs[:n_pieces], refs[n_pieces:]
    conv, (partial_ref, out_ref, w_ref, act_ref) = refs[:NX], refs[NX:]
    put_rows(table, pieces, w_ref, across=True)
    rows, wide = conv[0].shape[0] - 16, conv[0].shape[1]
    sums, gains = [], []
    for r in range(NX):
        edge = conv[r][rows : rows + 16, :].astype(F32)
        sums.append(conv[r][0:rows, :].astype(F32) + (edge[0:1] + edge[2:3] + edge[4:5]))
        gains.append(edge[1:2] + edge[3:4] + edge[5:6])
    centre = sum(jnp.sum(s, axis=1, keepdims=True) for s in sums) * (1.0 / CONV_CH)
    centred = [s - centre for s in sums]
    variance = sum(jnp.sum(s * s, axis=1, keepdims=True) for s in centred) * (1.0 / CONV_CH)
    scale = lax.rsqrt(variance + EPS)
    for r in range(NX):
        value = centred[r] * scale * gains[r]
        act_ref[:, r * wide : (r + 1) * wide] = (value * jax.nn.sigmoid(value)).astype(BF16)

    def tile(i, _):
        at = pl.multiple_of(i * 256, 256)
        out = lax.dot_general(
            act_ref[...], w_ref[pl.ds(at, 256), :], (((1,), (1,)), ((), ())), preferred_element_type=F32
        )
        out_ref[:, pl.ds(at, 256)] = (out + partial_ref[:, pl.ds(at, 256)]).astype(BF16)
        return 0

    lax.fori_loop(0, out_ref.shape[1] // 256, tile, 0)


def cost(flops, moved):
    return pl.CostEstimate(flops=flops, bytes_accessed=moved, transcendentals=0)


def shards(
    tokens, norm_gain, w_query, w_key, w_value, w_content, w_gate, sink_logit,
    conv_weight, conv_bias, channel_gain, out_attn, out_conv,
):
    count = tokens.shape[0]
    n_qkv = w_query.shape[1] + w_key.shape[1] + w_value.shape[1]
    n_in = n_qkv + w_content.shape[1] + w_gate.shape[1]

    wide = out_attn.shape[0]
    own_in = jnp.concatenate([w_query, w_key, w_value, w_content, w_gate, out_conv.T], 1)
    lines = around_y(own_in, OWN)
    beside = around_x([out_attn.T] * NX)
    prior = lax.ppermute(tokens[count - WINDOW :], SP, [(i, i + 1) for i in range(63)])
    width_1, width_2 = n_qkv + wide, n_in - n_qkv + wide
    plan = []
    for k in range(4):
        plan.append((0, 32 * k, 0, k, 0, 0, 32, n_qkv))
        plan.append((0, 32 * k, n_qkv, 4 + k, 0, 0, 32, wide))
        plan.append((1, 32 * k, 0, k, 0, n_qkv, 32, width_2))
    mine = copied([v for v, _ in lines] + beside, plan, [(128, width_1), (128, width_2)])
    table = sum((t for _, t in lines), [])
    parts = []
    for k, part in enumerate(mine, 1):
        block = join([(part, table), to_partner(part, table)])
        got = go_round(*block, "z")
        far = join(got[:3])
        parts.append([block, far, got[3], to_partner(*far)])
    qkv_parts, cg_parts = parts

    plan, table = [], []
    marks = [(0, 1), (-1, 3), (-4, 1), (1, 3)]
    row = 0
    for piece, (first, count_z) in enumerate(marks):
        for n in range(count_z):
            at_z = first - n if first < 0 else first + n
            for h in range(2):
                for k in range(4):
                    plan.append((0, row, wide * k, piece, 256 * n + 128 * h + 32 * k, n_qkv, 32, wide))
                table.append((at_z, 0, h ^ (piece == 3), 0, 0))
                row += 32
    block = (copied([v for v, _ in qkv_parts], plan, [(row, 4 * wide)])[0], table)
    got = go_round(*block, "y")
    attn_parts = [block, got[0], got[1], to_partner(*got[0])]

    def cut(part, lo, hi):
        return part[0][lo:hi], part[1][lo // 32 : hi // 32]

    plan, table, row = [], [], 0
    for piece, lo, hi in ((0, 0, 128), (1, 0, 768), (2, 0, 128), (0, 128, 256), (2, 128, 256), (3, 0, 768)):
        plan.append((0, row, 0, piece, lo, n_in - n_qkv, hi - lo, wide))
        table += cg_parts[piece][1][lo // 32 : hi // 32]
        row += hi - lo
    full = (copied([v for v, _ in cg_parts], plan, [(row, wide)])[0], table)
    got_0 = onward(*full, "x")
    got_1 = onward(*cut(got_0, 0, row // 2), "x")
    conv_parts = [full, got_0, got_1, to_partner(*got_0), to_partner(*got_1)]

    scaled, inv_rms = kernel_call(
        prep_kernel,
        out_shape=(
            jax.ShapeDtypeStruct((WINDOW + count, tokens.shape[1]), BF16),
            jax.ShapeDtypeStruct((WINDOW + count, 128), F32),
        ),
        in_specs=vmem(3),
        out_specs=tuple(vmem(2)),
        compiler_params=params(4),
        cost_estimate=cost(1 << 30, 8 << 20),
    )(tokens, prior, norm_gain.reshape(1, -1))

    pieces = [v for v, _ in qkv_parts]
    queries, keys_values = kernel_call(
        functools.partial(qkv_kernel, tables(qkv_parts)),
        out_shape=(jax.ShapeDtypeStruct((WINDOW + count, 256), BF16),) * 2,
        in_specs=vmem(len(pieces) + 4),
        out_specs=tuple(vmem(2)),
        scratch_shapes=[pltpu.VMEM((2048, n_qkv), BF16)],
        compiler_params=params(8),
        cost_estimate=cost(2 * count * 2048 * 384, 8 << 20),
    )(*pieces, scaled, inv_rms, *rope_tables())
    glu = kernel_call(
        functools.partial(glu_kernel, tables(cg_parts)),
        out_shape=jax.ShapeDtypeStruct((WINDOW + count, 256), BF16),
        in_specs=vmem(len(cg_parts) + 2),
        out_specs=vmem(1)[0],
        scratch_shapes=[pltpu.VMEM((2048, n_in - n_qkv), BF16)],
        compiler_params=params(8),
        cost_estimate=cost(2 * count * 2048 * 512, 8 << 20),
    )(*[v for v, _ in cg_parts], scaled, inv_rms)

    share = count // NX
    attn_blocks = kernel_call(
        attention_kernel,
        out_shape=tuple([jax.ShapeDtypeStruct((share, 256), BF16)] * NX),
        in_specs=[SMEM] + vmem(2),
        out_specs=tuple(vmem(NX)),
        scratch_shapes=[pltpu.VMEM((2, WINDOW + count, 128), BF16)] * 2 + [pltpu.VMEM((count, 256), BF16)],
        compiler_params=params(8),
        cost_estimate=cost(2 * count * 2048 * 512, 8 << 20),
    )(sink_logit, queries, keys_values)
    attn_blocks = around_x(attn_blocks)

    conv_blocks = kernel_call(
        conv_kernel,
        out_shape=tuple([jax.ShapeDtypeStruct((share + 16, 256), BF16)] * NX),
        in_specs=vmem(4),
        out_specs=tuple(vmem(NX)),
        scratch_shapes=[pltpu.VMEM((8, count + 48, 256), F32), pltpu.VMEM((count, 256), BF16)],
        compiler_params=params(16),
        cost_estimate=cost(2 * count * 2048 * 512, 8 << 20),
    )(glu, conv_weight, conv_bias.reshape(1, -1), channel_gain.reshape(1, -1))
    conv_blocks = around_x(conv_blocks)

    partial_sum = kernel_call(
        functools.partial(out_attn_kernel, tables(attn_parts)),
        out_shape=jax.ShapeDtypeStruct((share, 2048), F32),
        in_specs=vmem(len(attn_parts) + NX),
        out_specs=vmem(1)[0],
        scratch_shapes=[pltpu.VMEM((2048, 1024), BF16), pltpu.VMEM((share, 1024), BF16)],
        compiler_params=params(8),
        cost_estimate=cost(256 * 2048 * 2048, 6 << 20),
    )(*[v for v, _ in attn_parts], *attn_blocks)
    return kernel_call(
        functools.partial(out_conv_kernel, tables(conv_parts)),
        out_shape=jax.ShapeDtypeStruct((share, 2048), BF16),
        in_specs=vmem(len(conv_parts) + NX + 1),
        out_specs=vmem(1)[0],
        scratch_shapes=[pltpu.VMEM((2048, 1024), BF16), pltpu.VMEM((share, 1024), BF16)],
        compiler_params=params(10),
        cost_estimate=cost(256 * 2048 * 2048, 6 << 20),
    )(*[v for v, _ in conv_parts], *conv_blocks, partial_sum)


def solution(mesh):
    torus = Mesh(mesh.devices.reshape(8, 4, 2, mesh.shape["tp"]), ("z", "y", "c", "x"))
    return jax.shard_map(
        shards,
        mesh=torus,
        in_specs=(
            P(SP, None), P(), P(SP, "x"), P(SP, "x"), P(SP, "x"), P(SP, "x"), P(SP, "x"), P("x"),
            P(None, "x"), P("x"), P("x"), P("x", SP), P("x", SP),
        ),
        out_specs=P((*SP, "x"), None),
        check_vma=False,
    )
```

```python
import functools

import jax
import jax.numpy as jnp
import numpy as np
from jax import lax
from jax.experimental import pallas as pl
from jax.experimental.pallas import tpu as pltpu
from jax.sharding import Mesh
from jax.sharding import PartitionSpec as P


HEAD_DIM = 64
CONV_CH = 1024
KERNEL = 31
WINDOW = 128
EPS = 1e-05
THETA = 10000.0
SP = ("z", "y", "c")
NX = 4
F32 = jnp.float32
UNROLL = 7
BF16 = jnp.bfloat16


OWN = [(0, 0, 0, 0, 0)]


def to_partner(v, table):
    out = lax.ppermute(v, "c", [(0, 1), (1, 0)])
    return out, [(-a, -b, d ^ 1, e, -f) for a, b, d, e, f in table]


def onward(v, table, axis):
    size = lax.axis_size(axis)
    route = []
    for i in range(size):
        up, down = (i + 1) % size, (i - 1) % size
        if axis == "x":
            route += [(i, up), (size + i, size + down)]
        else:
            route += [(i * 2, up * 2), (i * 2 + 1, down * 2 + 1)]
    out = lax.ppermute(v, ("c", "x") if axis == "x" else (axis, "c"), route)
    k = {"z": 0, "y": 1, "x": 4}[axis]
    return out, [t[:k] + (t[k] - 1,) + t[k + 1 :] for t in table]


def go_round(v, table, axis):
    got = []
    for _ in range(lax.axis_size(axis) // 2):
        v, table = onward(v, table, axis)
        got.append((v, table))
    return got


def copy_kernel(plan, n_in, *refs):
    sources, results = refs[:n_in], refs[n_in:]
    for out, row, lane, src, row_0, lane_0, rows, lanes in plan:
        results[out][row : row + rows, lane : lane + lanes] = sources[src][row_0 : row_0 + rows, lane_0 : lane_0 + lanes]


def copied(sources, plan, shapes):
    outs = kernel_call(
        functools.partial(copy_kernel, plan, len(sources)),
        out_shape=tuple(jax.ShapeDtypeStruct(shape, BF16) for shape in shapes),
        in_specs=vmem(len(sources)),
        out_specs=tuple(vmem(len(shapes))),
        compiler_params=params(4),
        cost_estimate=cost(1 << 20, 1 << 20),
    )(*sources)
    return list(outs)


def join(parts, lo=0, hi=None):
    hi = hi or parts[0][0].shape[1]
    plan, row = [], 0
    for k, (v, _) in enumerate(parts):
        plan.append((0, row, 0, k, 0, lo, v.shape[0], hi - lo))
        row += v.shape[0]
    out = copied([v for v, _ in parts], plan, [(row, hi - lo)])[0]
    return out, sum((t for _, t in parts), [])


def tables(parts):
    return tuple(tuple(t) for _, t in parts)


def shift(v, axis, r):
    size = lax.axis_size(axis)
    return lax.ppermute(v, axis, [(i, (i + r) % size) for i in range(size)])


def around_x(blocks):
    return [blocks[0]] + [shift(blocks[r], "x", r) for r in range(1, NX)]


def around_y(v, table):
    return [(v, table)] + [(shift(v, "y", r), [(a, b, d, e - r, f) for a, b, d, e, f in table]) for r in (1, 3, 2)]


def kernel_call(body, **keys):
    return pl.pallas_call(body, **keys)


def vmem(n):
    return [pl.BlockSpec(memory_space=pltpu.VMEM)] * n


SMEM = pl.BlockSpec(memory_space=pltpu.SMEM)


def params(mib):
    return pltpu.CompilerParams(vmem_limit_bytes=mib * 1024 * 1024)


def put_rows(table, piece_refs, w_ref, across=False):
    z, y, c = (lax.axis_index(a) for a in SP)
    s = 1 - 2 * c
    for ref, places in zip(piece_refs, table):
        width = min(w_ref.shape[1], ref.shape[1])
        lane = pl.multiple_of(((-s * places[0][4]) & 3) * width, 128) if across else 0
        for k, (a, b, d, e, _) in enumerate(places):
            block = ((z + s * a) & 7) * 8 + ((y + s * b + e) & 3) * 2 + (c ^ d)
            row = pl.multiple_of(block * 32, 32)
            w_ref[pl.ds(row, 32), pl.ds(lane, width)] = ref[32 * k : 32 * k + 32, 0:width]


def lane_is(shape, period, limit):
    return lax.broadcasted_iota(jnp.int32, shape, len(shape) - 1) % period < limit


def sp_place():
    return (lax.axis_index("z") * 4 + lax.axis_index("y")) * 2 + lax.axis_index("c")


def turn(x, cosine, sine):
    other = jnp.where(lane_is(x.shape, 64, 32), pltpu.roll(x, 96, 1), pltpu.roll(x, 32, 1))
    return x * cosine + other * sine


def prep_kernel(tokens_ref, gain_ref, scaled_ref, inv_ref):
    def scale(wide, i):
        rows = pl.ds(pl.multiple_of(i * 32, 32), 32)
        scaled_ref[rows, :] = (wide * gain_ref[...]).astype(BF16)
        mean = jnp.sum(wide * wide, axis=1, keepdims=True) * (1.0 / wide.shape[1])
        inv_ref[rows, :] = jnp.broadcast_to(lax.rsqrt(mean + EPS), (32, 128))

    def tile(i, _):
        scale(tokens_ref[pl.ds(pl.multiple_of(i * 32, 32), 32), :].astype(F32), i)
        return 0

    lax.fori_loop(0, tokens_ref.shape[0] // 32, tile, 0, unroll=2)


def rope_tables():
    half = HEAD_DIM // 2
    inverse = np.tile(1.0 / THETA ** (np.arange(half) * 2.0 / HEAD_DIM), 4)[None, :]
    steps = np.concatenate([np.arange(32), 1024 * np.arange(64), 32 * np.arange(40)])[:, None]
    return jnp.asarray(np.cos(steps * inverse), F32), jnp.asarray(np.sin(steps * inverse), F32)


def times_inv(out, inv):
    return jnp.concatenate([out[:, k : k + 128] * inv for k in range(0, out.shape[1], 128)], 1)


def qkv_kernel(table, *refs):
    n_pieces = len(table)
    pieces = refs[:n_pieces]
    x_ref, inv_ref, cos_ref, sin_ref, q_ref, kv_ref, w_ref = refs[n_pieces:]
    put_rows(table, pieces, w_ref)
    sp = sp_place()
    size = 256

    def tile(i, _):
        rows = pl.ds(pl.multiple_of(i * size, 128), size)
        out = jnp.dot(x_ref[rows, :], w_ref[...], preferred_element_type=F32)
        out = times_inv(out, inv_ref[rows, :])
        ca, sa = cos_ref[pl.ds(32 + sp, 1), :], sin_ref[pl.ds(32 + sp, 1), :]
        cl, sl = cos_ref[0:32, :], sin_ref[0:32, :]
        cosines, sines = [], []
        for j in range(size // 32):
            at = pl.ds(96 + i * (size // 32) + j, 1)
            cb, sb = cos_ref[at, :], sin_ref[at, :]
            ch, sh = ca * cb - sa * sb, sa * cb + ca * sb
            cosines.append(ch * cl - sh * sl)
            sines.append(sh * cl + ch * sl)
        cosine, sine = jnp.concatenate(cosines, 0), jnp.concatenate(sines, 0)
        sine = jnp.where(lane_is(sine.shape, 64, 32), -sine, sine)
        for p in range(2):
            turned = turn(out[:, p * 128 : p * 128 + 128], cosine, sine).astype(BF16)
            q_ref[rows, p * 128 : p * 128 + 128] = turned * BF16(HEAD_DIM**-0.5)
        kv = out[:, 256:384]
        vk = pltpu.roll(kv, 64, 1)
        first = lane_is(kv.shape, 128, 64)
        kv_ref[rows, 0:128] = turn(jnp.where(first, kv, vk), cosine, sine).astype(BF16)
        kv_ref[rows, 128:256] = jnp.where(first, vk, kv).astype(BF16)
        return 0

    lax.fori_loop(0, x_ref.shape[0] // size, tile, 0)


def glu_kernel(table, *refs):
    n_pieces = len(table)
    pieces = refs[:n_pieces]
    x_ref, inv_ref, kv_ref, glu_ref, tail_ref, w_ref = refs[n_pieces:]
    put_rows(table, pieces, w_ref)
    size = 256

    def tile(i, _):
        rows = pl.ds(pl.multiple_of(i * size, 128), size)
        out = jnp.dot(x_ref[rows, :], w_ref[...], preferred_element_type=F32)
        out = times_inv(out, inv_ref[rows, :])
        glu_ref[rows, :] = (out[:, :256] * jax.nn.sigmoid(out[:, 256:])).astype(BF16)
        return 0

    lax.fori_loop(0, x_ref.shape[0] // size, tile, 0)
    tail_ref[0:WINDOW, :] = kv_ref[kv_ref.shape[0] - WINDOW :, :]
    tail_ref[WINDOW:, :] = glu_ref[glu_ref.shape[0] - 32 :, :]


def half_zero(rows):
    first = lane_is(rows.shape, 128, 64)
    zero = jnp.zeros(rows.shape, BF16)
    return jnp.where(first, rows, zero), jnp.where(first, zero, rows)


def attend(q_pair, keys, values, allowed, sink_ref):
    outs = []
    for pair in range(2):
        q = q_pair(pair)
        total = None
        for half in range(2):
            scores = lax.dot_general(q, keys[half], (((1,), (1,)), ((), ())), preferred_element_type=F32)
            scores = jnp.where(allowed, scores, -1e30)
            sink = sink_ref[pair * 2 + half]
            top = jnp.maximum(jnp.max(scores, axis=1, keepdims=True), sink)
            weights = jnp.exp(scores - top)
            denominator = jnp.sum(weights, axis=1, keepdims=True) + jnp.exp(sink - top)
            probability = (weights * (1.0 / denominator)).astype(BF16)
            part = jnp.dot(probability, values[half], preferred_element_type=F32)
            total = part if total is None else total + part
        outs.append(total.astype(BF16))
    return outs


def in_window():
    query = lax.broadcasted_iota(jnp.int32, (128, 256), 0)
    key = lax.broadcasted_iota(jnp.int32, (128, 256), 1)
    return (key > query) & (key <= query + WINDOW), key


def attention_kernel(sink_ref, q_ref, kv_ref, out_ref, k_ref, v_ref):
    k_ref[0], k_ref[1] = half_zero(kv_ref[:, 0:128])
    v_ref[0], v_ref[1] = half_zero(kv_ref[:, 128:256])
    allowed, _ = in_window()

    def block(b, _):
        at = pl.multiple_of(b * 128, 128)
        before = pl.multiple_of(b * 128 - 128, 128)
        outs = attend(
            lambda pair: q_ref[pl.ds(at, 128), pair * 128 : pair * 128 + 128],
            [k_ref[half, pl.ds(before, 256), :] for half in range(2)],
            [v_ref[half, pl.ds(before, 256), :] for half in range(2)],
            allowed,
            sink_ref,
        )
        for pair, out in enumerate(outs):
            out_ref[pl.ds(at, 128), pair * 128 : pair * 128 + 128] = out
        return 0

    lax.fori_loop(1, q_ref.shape[0] // 128, block, 0, unroll=UNROLL)


def first_attention_kernel(sink_ref, q_ref, kv_ref, prior_ref, rest_ref, *block_refs):
    kv = jnp.concatenate([prior_ref[0:WINDOW, :], kv_ref[0:128, :]], 0)
    allowed, key = in_window()
    allowed = allowed & (key >= jnp.where(sp_place() == 0, WINDOW, 0))
    out = attend(
        lambda pair: q_ref[0:128, pair * 128 : pair * 128 + 128],
        half_zero(kv[:, 0:128]),
        half_zero(kv[:, 128:256]),
        allowed,
        sink_ref,
    )
    to_blocks(rest_ref, block_refs)
    for r, ref in enumerate(block_refs):

        @pl.when(((lax.axis_index("x") + r) & 3) == 0)
        def _(ref=ref):
            for pair in range(2):
                ref[0:128, pair * 128 : pair * 128 + 128] = out[pair]


def to_blocks(src_ref, block_refs):
    share = src_ref.shape[0] // NX
    for r, ref in enumerate(block_refs):
        at = pl.multiple_of(((lax.axis_index("x") + r) & 3) * share, share)
        ref[0:share, :] = src_ref[pl.ds(at, share), :]


def conv_kernel(glu_ref, prior_ref, w_ref, bias_ref, gain_ref, *refs):
    block_refs, (shift_ref, out_ref) = refs[:NX], refs[NX:]
    tokens = glu_ref.shape[0]
    shift_ref[0, 0:32, :] = prior_ref[WINDOW:, :].astype(F32)
    shift_ref[0, 32 : 32 + tokens, :] = glu_ref[...].astype(F32)

    def fill(i, _):
        at = pl.multiple_of(i * 32, 32)
        rows = shift_ref[0, pl.ds(at, 40), :]
        for b in range(1, 8):
            shift_ref[b, pl.ds(at, 32), :] = rows[b : b + 32, :]
        return 0

    lax.fori_loop(0, tokens // 32 + 1, fill, 0)

    def tile(i, _):
        at = pl.multiple_of(i * 32, 32)
        total = None
        for j in range(KERNEL):
            ahead, b = divmod(j + 2, 8)
            term = w_ref[j : j + 1, :] * shift_ref[b, pl.ds(at + ahead * 8, 32), :]
            total = term if total is None else total + term
        out_ref[pl.ds(at, 32), :] = total.astype(BF16)
        return 0

    lax.fori_loop(0, tokens // 32, tile, 0)
    to_blocks(out_ref, block_refs)
    edge = jnp.concatenate([bias_ref[...], gain_ref[...]], 0)
    high = edge.astype(BF16).astype(F32)
    middle = (edge - high).astype(BF16).astype(F32)
    low = edge - high - middle
    rows = jnp.concatenate([high, middle, low, jnp.zeros((16 - 3 * edge.shape[0], edge.shape[1]), F32)], 0).astype(BF16)
    for ref in block_refs:
        ref[ref.shape[0] - 16 :, :] = rows


def out_attn_kernel(table, *refs):
    n_pieces = len(table)
    pieces, refs = refs[:n_pieces], refs[n_pieces:]
    attn, (out_ref, w_ref, act_ref) = refs[:NX], refs[NX:]
    put_rows(table, pieces, w_ref)
    wide = attn[0].shape[1]
    for r in range(NX):
        act_ref[:, r * wide : (r + 1) * wide] = attn[r][...]

    def tile(i, _):
        at = pl.multiple_of(i * 256, 256)
        out_ref[:, pl.ds(at, 256)] = lax.dot_general(
            act_ref[...], w_ref[pl.ds(at, 256), :], (((1,), (1,)), ((), ())), preferred_element_type=F32
        )
        return 0

    lax.fori_loop(0, out_ref.shape[1] // 256, tile, 0)


def out_conv_kernel(table, *refs):
    n_pieces = len(table)
    pieces, refs = refs[:n_pieces], refs[n_pieces:]
    conv, (partial_ref, out_ref, w_ref, act_ref) = refs[:NX], refs[NX:]
    put_rows(table, pieces, w_ref, across=True)
    rows, wide = conv[0].shape[0] - 16, conv[0].shape[1]
    sums, gains = [], []
    for r in range(NX):
        edge = conv[r][rows : rows + 16, :].astype(F32)
        sums.append(conv[r][0:rows, :].astype(F32) + (edge[0:1] + edge[2:3] + edge[4:5]))
        gains.append(edge[1:2] + edge[3:4] + edge[5:6])
    centre = sum(jnp.sum(s, axis=1, keepdims=True) for s in sums) * (1.0 / CONV_CH)
    centred = [s - centre for s in sums]
    variance = sum(jnp.sum(s * s, axis=1, keepdims=True) for s in centred) * (1.0 / CONV_CH)
    scale = lax.rsqrt(variance + EPS)
    for r in range(NX):
        value = centred[r] * scale * gains[r]
        act_ref[:, r * wide : (r + 1) * wide] = (value * jax.nn.sigmoid(value)).astype(BF16)

    def tile(i, _):
        at = pl.multiple_of(i * 256, 256)
        out = lax.dot_general(
            act_ref[...], w_ref[pl.ds(at, 256), :], (((1,), (1,)), ((), ())), preferred_element_type=F32
        )
        out_ref[:, pl.ds(at, 256)] = (out + partial_ref[:, pl.ds(at, 256)]).astype(BF16)
        return 0

    lax.fori_loop(0, out_ref.shape[1] // 256, tile, 0)


def cost(flops, moved):
    return pl.CostEstimate(flops=flops, bytes_accessed=moved, transcendentals=0)


def shards(
    tokens, norm_gain, w_query, w_key, w_value, w_content, w_gate, sink_logit,
    conv_weight, conv_bias, channel_gain, out_attn, out_conv,
):
    count = tokens.shape[0]
    n_qkv = w_query.shape[1] + w_key.shape[1] + w_value.shape[1]
    n_in = n_qkv + w_content.shape[1] + w_gate.shape[1]

    wide = out_attn.shape[0]
    own_in = jnp.concatenate([w_query, w_key, w_value, w_content, w_gate, out_conv.T], 1)
    lines = around_y(own_in, OWN)
    beside = around_x([out_attn.T] * NX)
    width_1, width_2 = n_qkv + wide, n_in - n_qkv + wide
    plan = []
    for k in range(4):
        plan.append((0, 32 * k, 0, k, 0, 0, 32, n_qkv))
        plan.append((0, 32 * k, n_qkv, 4 + k, 0, 0, 32, wide))
        plan.append((1, 32 * k, 0, k, 0, n_qkv, 32, width_2))
    mine = copied([v for v, _ in lines] + beside, plan, [(128, width_1), (128, width_2)])
    table = sum((t for _, t in lines), [])
    parts = []
    for k, part in enumerate(mine, 1):
        block = join([(part, table), to_partner(part, table)])
        got = go_round(*block, "z")
        far = join(got[:3])
        parts.append([block, far, got[3], to_partner(*far)])
    qkv_parts, cg_parts = parts

    plan, table = [], []
    marks = [(0, 1), (-1, 3), (-4, 1), (1, 3)]
    row = 0
    for piece, (first, count_z) in enumerate(marks):
        for n in range(count_z):
            at_z = first - n if first < 0 else first + n
            for h in range(2):
                for k in range(4):
                    plan.append((0, row, wide * k, piece, 256 * n + 128 * h + 32 * k, n_qkv, 32, wide))
                table.append((at_z, 0, h ^ (piece == 3), 0, 0))
                row += 32
    block = (copied([v for v, _ in qkv_parts], plan, [(row, 4 * wide)])[0], table)
    got = go_round(*block, "y")
    attn_parts = [block, got[0], got[1], to_partner(*got[0])]

    def cut(part, lo, hi):
        return part[0][lo:hi], part[1][lo // 32 : hi // 32]

    plan, table, row = [], [], 0
    for piece, lo, hi in ((0, 0, 128), (1, 0, 768), (2, 0, 128), (0, 128, 256), (2, 128, 256), (3, 0, 768)):
        plan.append((0, row, 0, piece, lo, n_in - n_qkv, hi - lo, wide))
        table += cg_parts[piece][1][lo // 32 : hi // 32]
        row += hi - lo
    full = (copied([v for v, _ in cg_parts], plan, [(row, wide)])[0], table)
    got_0 = onward(*full, "x")
    got_1 = onward(*cut(got_0, 0, row // 2), "x")
    conv_parts = [full, got_0, got_1, to_partner(*got_0), to_partner(*got_1)]

    scaled, inv_rms = kernel_call(
        prep_kernel,
        out_shape=(
            jax.ShapeDtypeStruct(tokens.shape, BF16),
            jax.ShapeDtypeStruct((count, 128), F32),
        ),
        in_specs=vmem(2),
        out_specs=tuple(vmem(2)),
        compiler_params=params(4),
        cost_estimate=cost(1 << 30, 8 << 20),
    )(tokens, norm_gain.reshape(1, -1))

    pieces = [v for v, _ in qkv_parts]
    queries, keys_values = kernel_call(
        functools.partial(qkv_kernel, tables(qkv_parts)),
        out_shape=(jax.ShapeDtypeStruct((count, 256), BF16),) * 2,
        in_specs=vmem(len(pieces) + 4),
        out_specs=tuple(vmem(2)),
        scratch_shapes=[pltpu.VMEM((2048, n_qkv), BF16)],
        compiler_params=params(8),
        cost_estimate=cost(2 * count * 2048 * 384, 8 << 20),
    )(*pieces, scaled, inv_rms, *rope_tables())
    glu, tail = kernel_call(
        functools.partial(glu_kernel, tables(cg_parts)),
        out_shape=(jax.ShapeDtypeStruct((count, 256), BF16), jax.ShapeDtypeStruct((WINDOW + 32, 256), BF16)),
        in_specs=vmem(len(cg_parts) + 3),
        out_specs=tuple(vmem(2)),
        scratch_shapes=[pltpu.VMEM((2048, n_in - n_qkv), BF16)],
        compiler_params=params(8),
        cost_estimate=cost(2 * count * 2048 * 512, 8 << 20),
    )(*[v for v, _ in cg_parts], scaled, inv_rms, keys_values)
    prior = lax.ppermute(tail, SP, [(i, i + 1) for i in range(63)])

    share = count // NX
    attended = kernel_call(
        attention_kernel,
        out_shape=jax.ShapeDtypeStruct((count, 256), BF16),
        in_specs=[SMEM] + vmem(2),
        out_specs=vmem(1)[0],
        scratch_shapes=[pltpu.VMEM((2, count, 128), BF16)] * 2,
        compiler_params=params(8),
        cost_estimate=cost(2 * count * 2048 * 512, 8 << 20),
    )(sink_logit, queries, keys_values)
    attn_blocks = kernel_call(
        first_attention_kernel,
        out_shape=tuple([jax.ShapeDtypeStruct((share, 256), BF16)] * NX),
        in_specs=[SMEM] + vmem(4),
        out_specs=tuple(vmem(NX)),
        compiler_params=params(4),
        cost_estimate=cost(1 << 30, 1 << 20),
    )(sink_logit, queries, keys_values, prior, attended)
    attn_blocks = around_x(attn_blocks)

    conv_blocks = kernel_call(
        conv_kernel,
        out_shape=tuple([jax.ShapeDtypeStruct((share + 16, 256), BF16)] * NX),
        in_specs=vmem(5),
        out_specs=tuple(vmem(NX)),
        scratch_shapes=[pltpu.VMEM((8, count + 48, 256), F32), pltpu.VMEM((count, 256), BF16)],
        compiler_params=params(16),
        cost_estimate=cost(2 * count * 2048 * 512, 8 << 20),
    )(glu, prior, conv_weight, conv_bias.reshape(1, -1), channel_gain.reshape(1, -1))
    conv_blocks = around_x(conv_blocks)

    partial_sum = kernel_call(
        functools.partial(out_attn_kernel, tables(attn_parts)),
        out_shape=jax.ShapeDtypeStruct((share, 2048), F32),
        in_specs=vmem(len(attn_parts) + NX),
        out_specs=vmem(1)[0],
        scratch_shapes=[pltpu.VMEM((2048, 1024), BF16), pltpu.VMEM((share, 1024), BF16)],
        compiler_params=params(8),
        cost_estimate=cost(256 * 2048 * 2048, 6 << 20),
    )(*[v for v, _ in attn_parts], *attn_blocks)
    return kernel_call(
        functools.partial(out_conv_kernel, tables(conv_parts)),
        out_shape=jax.ShapeDtypeStruct((share, 2048), BF16),
        in_specs=vmem(len(conv_parts) + NX + 1),
        out_specs=vmem(1)[0],
        scratch_shapes=[pltpu.VMEM((2048, 1024), BF16), pltpu.VMEM((share, 1024), BF16)],
        compiler_params=params(10),
        cost_estimate=cost(256 * 2048 * 2048, 6 << 20),
    )(*[v for v, _ in conv_parts], *conv_blocks, partial_sum)


def solution(mesh):
    torus = Mesh(mesh.devices.reshape(8, 4, 2, mesh.shape["tp"]), ("z", "y", "c", "x"))
    return jax.shard_map(
        shards,
        mesh=torus,
        in_specs=(
            P(SP, None), P(), P(SP, "x"), P(SP, "x"), P(SP, "x"), P(SP, "x"), P(SP, "x"), P("x"),
            P(None, "x"), P("x"), P("x"), P("x", SP), P("x", SP),
        ),
        out_specs=P((*SP, "x"), None),
        check_vma=False,
    )
```

```python
import functools

import jax
import jax.numpy as jnp
import numpy as np
from jax import lax
from jax.experimental import pallas as pl
from jax.experimental.pallas import tpu as pltpu
from jax.sharding import Mesh
from jax.sharding import PartitionSpec as P


HEAD_DIM = 64
CONV_CH = 1024
KERNEL = 31
WINDOW = 128
EPS = 1e-05
THETA = 10000.0
SP = ("z", "y", "c")
NX = 4
F32 = jnp.float32
UNROLL = 7
BF16 = jnp.bfloat16


OWN = [(0, 0, 0, 0, 0)]


def to_partner(v, table):
    out = lax.ppermute(v, "c", [(0, 1), (1, 0)])
    return out, [(-a, -b, d ^ 1, e, -f) for a, b, d, e, f in table]


def onward(v, table, axis):
    size = lax.axis_size(axis)
    route = []
    for i in range(size):
        up, down = (i + 1) % size, (i - 1) % size
        if axis == "x":
            route += [(i, up), (size + i, size + down)]
        else:
            route += [(i * 2, up * 2), (i * 2 + 1, down * 2 + 1)]
    out = lax.ppermute(v, ("c", "x") if axis == "x" else (axis, "c"), route)
    k = {"z": 0, "y": 1, "x": 4}[axis]
    return out, [t[:k] + (t[k] - 1,) + t[k + 1 :] for t in table]


def go_round(v, table, axis):
    got = []
    for _ in range(lax.axis_size(axis) // 2):
        v, table = onward(v, table, axis)
        got.append((v, table))
    return got


def copy_kernel(plan, n_in, *refs):
    sources, results = refs[:n_in], refs[n_in:]
    for out, row, lane, src, row_0, lane_0, rows, lanes in plan:
        results[out][row : row + rows, lane : lane + lanes] = sources[src][row_0 : row_0 + rows, lane_0 : lane_0 + lanes]


def copied(sources, plan, shapes):
    outs = kernel_call(
        functools.partial(copy_kernel, plan, len(sources)),
        out_shape=tuple(jax.ShapeDtypeStruct(shape, BF16) for shape in shapes),
        in_specs=vmem(len(sources)),
        out_specs=tuple(vmem(len(shapes))),
        compiler_params=params(4),
        cost_estimate=cost(1 << 20, 1 << 20),
    )(*sources)
    return list(outs)


def join(parts, lo=0, hi=None):
    hi = hi or parts[0][0].shape[1]
    plan, row = [], 0
    for k, (v, _) in enumerate(parts):
        plan.append((0, row, 0, k, 0, lo, v.shape[0], hi - lo))
        row += v.shape[0]
    out = copied([v for v, _ in parts], plan, [(row, hi - lo)])[0]
    return out, sum((t for _, t in parts), [])


def tables(parts):
    return tuple(tuple(t) for _, t in parts)


def shift(v, axis, r):
    size = lax.axis_size(axis)
    return lax.ppermute(v, axis, [(i, (i + r) % size) for i in range(size)])


def around_x(blocks):
    return [blocks[0]] + [shift(blocks[r], "x", r) for r in range(1, NX)]


def around_y(v, table):
    return [(v, table)] + [(shift(v, "y", r), [(a, b, d, e - r, f) for a, b, d, e, f in table]) for r in (1, 3, 2)]


def kernel_call(body, **keys):
    return pl.pallas_call(body, **keys)


def vmem(n):
    return [pl.BlockSpec(memory_space=pltpu.VMEM)] * n


SMEM = pl.BlockSpec(memory_space=pltpu.SMEM)


def params(mib):
    return pltpu.CompilerParams(vmem_limit_bytes=mib * 1024 * 1024)


def put_rows(table, piece_refs, w_ref, across=False):
    z, y, c = (lax.axis_index(a) for a in SP)
    s = 1 - 2 * c
    for ref, places in zip(piece_refs, table):
        width = min(w_ref.shape[1], ref.shape[1])
        lane = pl.multiple_of(((-s * places[0][4]) & 3) * width, 128) if across else 0
        for k, (a, b, d, e, _) in enumerate(places):
            block = ((z + s * a) & 7) * 8 + ((y + s * b + e) & 3) * 2 + (c ^ d)
            row = pl.multiple_of(block * 32, 32)
            w_ref[pl.ds(row, 32), pl.ds(lane, width)] = ref[32 * k : 32 * k + 32, 0:width]


def lane_is(shape, period, limit):
    return lax.broadcasted_iota(jnp.int32, shape, len(shape) - 1) % period < limit


def sp_place():
    return (lax.axis_index("z") * 4 + lax.axis_index("y")) * 2 + lax.axis_index("c")


def turn(x, cosine, sine):
    other = jnp.where(lane_is(x.shape, 64, 32), pltpu.roll(x, 96, 1), pltpu.roll(x, 32, 1))
    return x * cosine + other * sine


def prep_kernel(tokens_ref, gain_ref, scaled_ref, inv_ref):
    def scale(wide, i):
        rows = pl.ds(pl.multiple_of(i * 32, 32), 32)
        scaled_ref[rows, :] = (wide * gain_ref[...]).astype(BF16)
        mean = jnp.sum(wide * wide, axis=1, keepdims=True) * (1.0 / wide.shape[1])
        inv_ref[rows, :] = jnp.broadcast_to(lax.rsqrt(mean + EPS), (32, 128))

    def tile(i, _):
        scale(tokens_ref[pl.ds(pl.multiple_of(i * 32, 32), 32), :].astype(F32), i)
        return 0

    lax.fori_loop(0, tokens_ref.shape[0] // 32, tile, 0, unroll=2)


def rope_tables():
    half = HEAD_DIM // 2
    inverse = np.tile(1.0 / THETA ** (np.arange(half) * 2.0 / HEAD_DIM), 4)[None, :]
    steps = np.concatenate([np.arange(32), 1024 * np.arange(64), 32 * np.arange(40)])[:, None]
    return jnp.asarray(np.cos(steps * inverse), F32), jnp.asarray(np.sin(steps * inverse), F32)


def times_inv(out, inv):
    return jnp.concatenate([out[:, k : k + 128] * inv for k in range(0, out.shape[1], 128)], 1)


def qkv_kernel(table, *refs):
    n_pieces = len(table)
    pieces = refs[:n_pieces]
    x_ref, inv_ref, cos_ref, sin_ref, q_ref, kv_ref, w_ref = refs[n_pieces:]
    put_rows(table, pieces, w_ref)
    sp = sp_place()
    size = 1024

    def tile(i, _):
        rows = pl.ds(pl.multiple_of(i * size, 128), size)
        out = jnp.dot(x_ref[rows, :], w_ref[...], preferred_element_type=F32)
        out = times_inv(out, inv_ref[rows, :])
        ca, sa = cos_ref[pl.ds(32 + sp, 1), :], sin_ref[pl.ds(32 + sp, 1), :]
        cl, sl = cos_ref[0:32, :], sin_ref[0:32, :]
        cosines, sines = [], []
        for j in range(size // 32):
            at = pl.ds(96 + i * (size // 32) + j, 1)
            cb, sb = cos_ref[at, :], sin_ref[at, :]
            ch, sh = ca * cb - sa * sb, sa * cb + ca * sb
            cosines.append(ch * cl - sh * sl)
            sines.append(sh * cl + ch * sl)
        cosine, sine = jnp.concatenate(cosines, 0), jnp.concatenate(sines, 0)
        sine = jnp.where(lane_is(sine.shape, 64, 32), -sine, sine)
        for p in range(2):
            turned = turn(out[:, p * 128 : p * 128 + 128], cosine, sine).astype(BF16)
            q_ref[rows, p * 128 : p * 128 + 128] = turned * BF16(HEAD_DIM**-0.5)
        kv = out[:, 256:384]
        vk = pltpu.roll(kv, 64, 1)
        first = lane_is(kv.shape, 128, 64)
        kv_ref[rows, 0:128] = turn(jnp.where(first, kv, vk), cosine, sine).astype(BF16)
        kv_ref[rows, 128:256] = jnp.where(first, vk, kv).astype(BF16)
        return 0

    lax.fori_loop(0, x_ref.shape[0] // size, tile, 0)


def glu_kernel(table, *refs):
    n_pieces = len(table)
    pieces = refs[:n_pieces]
    x_ref, inv_ref, kv_ref, glu_ref, tail_ref, w_ref = refs[n_pieces:]
    put_rows(table, pieces, w_ref)
    size = 1024

    def tile(i, _):
        rows = pl.ds(pl.multiple_of(i * size, 128), size)
        out = jnp.dot(x_ref[rows, :], w_ref[...], preferred_element_type=F32)
        out = times_inv(out, inv_ref[rows, :])
        glu_ref[rows, :] = (out[:, :256] * jax.nn.sigmoid(out[:, 256:])).astype(BF16)
        return 0

    lax.fori_loop(0, x_ref.shape[0] // size, tile, 0)
    tail_ref[0:WINDOW, :] = kv_ref[kv_ref.shape[0] - WINDOW :, :]
    tail_ref[WINDOW:, :] = glu_ref[glu_ref.shape[0] - 32 :, :]


def half_zero(rows):
    first = lane_is(rows.shape, 128, 64)
    zero = jnp.zeros(rows.shape, BF16)
    return jnp.where(first, rows, zero), jnp.where(first, zero, rows)


def attend(q_pair, keys, values, allowed, sink_ref):
    outs = []
    for pair in range(2):
        q = q_pair(pair)
        total = None
        for half in range(2):
            scores = lax.dot_general(q, keys[half], (((1,), (1,)), ((), ())), preferred_element_type=F32)
            scores = jnp.where(allowed, scores, -1e30)
            sink = sink_ref[pair * 2 + half]
            top = jnp.maximum(jnp.max(scores, axis=1, keepdims=True), sink)
            weights = jnp.exp(scores - top)
            denominator = jnp.sum(weights, axis=1, keepdims=True) + jnp.exp(sink - top)
            probability = (weights * (1.0 / denominator)).astype(BF16)
            part = jnp.dot(probability, values[half], preferred_element_type=F32)
            total = part if total is None else total + part
        outs.append(total.astype(BF16))
    return outs


def in_window():
    query = lax.broadcasted_iota(jnp.int32, (128, 256), 0)
    key = lax.broadcasted_iota(jnp.int32, (128, 256), 1)
    return (key > query) & (key <= query + WINDOW), key


def attention_kernel(sink_ref, q_ref, kv_ref, out_ref, k_ref, v_ref):
    k_ref[0], k_ref[1] = half_zero(kv_ref[:, 0:128])
    v_ref[0], v_ref[1] = half_zero(kv_ref[:, 128:256])
    allowed, _ = in_window()

    def block(b, _):
        at = pl.multiple_of(b * 128, 128)
        before = pl.multiple_of(b * 128 - 128, 128)
        outs = attend(
            lambda pair: q_ref[pl.ds(at, 128), pair * 128 : pair * 128 + 128],
            [k_ref[half, pl.ds(before, 256), :] for half in range(2)],
            [v_ref[half, pl.ds(before, 256), :] for half in range(2)],
            allowed,
            sink_ref,
        )
        for pair, out in enumerate(outs):
            out_ref[pl.ds(at, 128), pair * 128 : pair * 128 + 128] = out
        return 0

    lax.fori_loop(1, q_ref.shape[0] // 128, block, 0, unroll=UNROLL)


def first_attention_kernel(sink_ref, q_ref, kv_ref, prior_ref, rest_ref, *block_refs):
    kv = jnp.concatenate([prior_ref[0:WINDOW, :], kv_ref[0:128, :]], 0)
    allowed, key = in_window()
    allowed = allowed & (key >= jnp.where(sp_place() == 0, WINDOW, 0))
    out = attend(
        lambda pair: q_ref[0:128, pair * 128 : pair * 128 + 128],
        half_zero(kv[:, 0:128]),
        half_zero(kv[:, 128:256]),
        allowed,
        sink_ref,
    )
    to_blocks(rest_ref, block_refs)
    for r, ref in enumerate(block_refs):

        @pl.when(((lax.axis_index("x") + r) & 3) == 0)
        def _(ref=ref):
            for pair in range(2):
                ref[0:128, pair * 128 : pair * 128 + 128] = out[pair]


def to_blocks(src_ref, block_refs):
    share = src_ref.shape[0] // NX
    for r, ref in enumerate(block_refs):
        at = pl.multiple_of(((lax.axis_index("x") + r) & 3) * share, share)
        ref[0:share, :] = src_ref[pl.ds(at, share), :]


def conv_kernel(glu_ref, prior_ref, w_ref, bias_ref, gain_ref, *refs):
    block_refs, (shift_ref, out_ref) = refs[:NX], refs[NX:]
    tokens = glu_ref.shape[0]
    shift_ref[0, 0:32, :] = prior_ref[WINDOW:, :].astype(F32)
    shift_ref[0, 32 : 32 + tokens, :] = glu_ref[...].astype(F32)

    def fill(i, _):
        at = pl.multiple_of(i * 32, 32)
        rows = shift_ref[0, pl.ds(at, 40), :]
        for b in range(1, 8):
            shift_ref[b, pl.ds(at, 32), :] = rows[b : b + 32, :]
        return 0

    lax.fori_loop(0, tokens // 32 + 1, fill, 0, unroll=3)

    def tile(i, _):
        at = pl.multiple_of(i * 32, 32)
        total = None
        for j in range(KERNEL):
            ahead, b = divmod(j + 2, 8)
            term = w_ref[j : j + 1, :] * shift_ref[b, pl.ds(at + ahead * 8, 32), :]
            total = term if total is None else total + term
        out_ref[pl.ds(at, 32), :] = total.astype(BF16)
        return 0

    lax.fori_loop(0, tokens // 32, tile, 0, unroll=4)
    to_blocks(out_ref, block_refs)
    edge = jnp.concatenate([bias_ref[...], gain_ref[...]], 0)
    high = edge.astype(BF16).astype(F32)
    middle = (edge - high).astype(BF16).astype(F32)
    low = edge - high - middle
    rows = jnp.concatenate([high, middle, low, jnp.zeros((16 - 3 * edge.shape[0], edge.shape[1]), F32)], 0).astype(BF16)
    for ref in block_refs:
        ref[ref.shape[0] - 16 :, :] = rows


def out_attn_kernel(table, *refs):
    n_pieces = len(table)
    pieces, refs = refs[:n_pieces], refs[n_pieces:]
    attn, (out_ref, w_ref, act_ref) = refs[:NX], refs[NX:]
    put_rows(table, pieces, w_ref)
    wide = attn[0].shape[1]
    for r in range(NX):
        act_ref[:, r * wide : (r + 1) * wide] = attn[r][...]

    def tile(i, _):
        at = pl.multiple_of(i * 1024, 1024)
        out_ref[:, pl.ds(at, 1024)] = lax.dot_general(
            act_ref[...], w_ref[pl.ds(at, 1024), :], (((1,), (1,)), ((), ())), preferred_element_type=F32
        )
        return 0

    lax.fori_loop(0, out_ref.shape[1] // 1024, tile, 0)


def out_conv_kernel(table, *refs):
    n_pieces = len(table)
    pieces, refs = refs[:n_pieces], refs[n_pieces:]
    conv, (partial_ref, out_ref, w_ref, act_ref) = refs[:NX], refs[NX:]
    put_rows(table, pieces, w_ref, across=True)
    rows, wide = conv[0].shape[0] - 16, conv[0].shape[1]
    sums, gains = [], []
    for r in range(NX):
        edge = conv[r][rows : rows + 16, :].astype(F32)
        sums.append(conv[r][0:rows, :].astype(F32) + (edge[0:1] + edge[2:3] + edge[4:5]))
        gains.append(edge[1:2] + edge[3:4] + edge[5:6])
    centre = sum(jnp.sum(s, axis=1, keepdims=True) for s in sums) * (1.0 / CONV_CH)
    centred = [s - centre for s in sums]
    variance = sum(jnp.sum(s * s, axis=1, keepdims=True) for s in centred) * (1.0 / CONV_CH)
    scale = lax.rsqrt(variance + EPS)
    for r in range(NX):
        value = centred[r] * scale * gains[r]
        act_ref[:, r * wide : (r + 1) * wide] = (value * jax.nn.sigmoid(value)).astype(BF16)

    def tile(i, _):
        at = pl.multiple_of(i * 1024, 1024)
        out = lax.dot_general(
            act_ref[...], w_ref[pl.ds(at, 1024), :], (((1,), (1,)), ((), ())), preferred_element_type=F32
        )
        out_ref[:, pl.ds(at, 1024)] = (out + partial_ref[:, pl.ds(at, 1024)]).astype(BF16)
        return 0

    lax.fori_loop(0, out_ref.shape[1] // 1024, tile, 0)


def cost(flops, moved):
    return pl.CostEstimate(flops=flops, bytes_accessed=moved, transcendentals=0)


def shards(
    tokens, norm_gain, w_query, w_key, w_value, w_content, w_gate, sink_logit,
    conv_weight, conv_bias, channel_gain, out_attn, out_conv,
):
    count = tokens.shape[0]
    n_qkv = w_query.shape[1] + w_key.shape[1] + w_value.shape[1]
    n_in = n_qkv + w_content.shape[1] + w_gate.shape[1]

    wide = out_attn.shape[0]
    own_in = jnp.concatenate([w_query, w_key, w_value, w_content, w_gate, out_conv.T], 1)
    lines = around_y(own_in, OWN)
    beside = around_x([out_attn.T] * NX)
    width_1, width_2 = n_qkv + wide, n_in - n_qkv + wide
    plan = []
    for k in range(4):
        plan.append((0, 32 * k, 0, k, 0, 0, 32, n_qkv))
        plan.append((0, 32 * k, n_qkv, 4 + k, 0, 0, 32, wide))
        plan.append((1, 32 * k, 0, k, 0, n_qkv, 32, width_2))
    mine = copied([v for v, _ in lines] + beside, plan, [(128, width_1), (128, width_2)])
    table = sum((t for _, t in lines), [])
    parts = []
    for k, part in enumerate(mine, 1):
        block = join([(part, table), to_partner(part, table)])
        got = go_round(*block, "z")
        far = join(got[:3])
        parts.append([block, far, got[3], to_partner(*far)])
    qkv_parts, cg_parts = parts

    plan, table = [], []
    marks = [(0, 1), (-1, 3), (-4, 1), (1, 3)]
    row = 0
    for piece, (first, count_z) in enumerate(marks):
        for n in range(count_z):
            at_z = first - n if first < 0 else first + n
            for h in range(2):
                for k in range(4):
                    plan.append((0, row, wide * k, piece, 256 * n + 128 * h + 32 * k, n_qkv, 32, wide))
                table.append((at_z, 0, h ^ (piece == 3), 0, 0))
                row += 32
    block = (copied([v for v, _ in qkv_parts], plan, [(row, 4 * wide)])[0], table)
    got = go_round(*block, "y")
    attn_parts = [block, got[0], got[1], to_partner(*got[0])]

    def cut(part, lo, hi):
        return part[0][lo:hi], part[1][lo // 32 : hi // 32]

    plan, table, row = [], [], 0
    for piece, lo, hi in ((0, 0, 128), (1, 0, 768), (2, 0, 128), (0, 128, 256), (2, 128, 256), (3, 0, 768)):
        plan.append((0, row, 0, piece, lo, n_in - n_qkv, hi - lo, wide))
        table += cg_parts[piece][1][lo // 32 : hi // 32]
        row += hi - lo
    full = (copied([v for v, _ in cg_parts], plan, [(row, wide)])[0], table)
    got_0 = onward(*full, "x")
    got_1 = onward(*cut(got_0, 0, row // 2), "x")
    conv_parts = [full, got_0, got_1, to_partner(*got_0), to_partner(*got_1)]

    scaled, inv_rms = kernel_call(
        prep_kernel,
        out_shape=(
            jax.ShapeDtypeStruct(tokens.shape, BF16),
            jax.ShapeDtypeStruct((count, 128), F32),
        ),
        in_specs=vmem(2),
        out_specs=tuple(vmem(2)),
        compiler_params=params(4),
        cost_estimate=cost(1 << 30, 8 << 20),
    )(tokens, norm_gain.reshape(1, -1))

    pieces = [v for v, _ in qkv_parts]
    queries, keys_values = kernel_call(
        functools.partial(qkv_kernel, tables(qkv_parts)),
        out_shape=(jax.ShapeDtypeStruct((count, 256), BF16),) * 2,
        in_specs=vmem(len(pieces) + 4),
        out_specs=tuple(vmem(2)),
        scratch_shapes=[pltpu.VMEM((2048, n_qkv), BF16)],
        compiler_params=params(8),
        cost_estimate=cost(2 * count * 2048 * 384, 8 << 20),
    )(*pieces, scaled, inv_rms, *rope_tables())
    glu, tail = kernel_call(
        functools.partial(glu_kernel, tables(cg_parts)),
        out_shape=(jax.ShapeDtypeStruct((count, 256), BF16), jax.ShapeDtypeStruct((WINDOW + 32, 256), BF16)),
        in_specs=vmem(len(cg_parts) + 3),
        out_specs=tuple(vmem(2)),
        scratch_shapes=[pltpu.VMEM((2048, n_in - n_qkv), BF16)],
        compiler_params=params(8),
        cost_estimate=cost(2 * count * 2048 * 512, 8 << 20),
    )(*[v for v, _ in cg_parts], scaled, inv_rms, keys_values)
    prior = lax.ppermute(tail, SP, [(i, i + 1) for i in range(63)])

    share = count // NX
    attended = kernel_call(
        attention_kernel,
        out_shape=jax.ShapeDtypeStruct((count, 256), BF16),
        in_specs=[SMEM] + vmem(2),
        out_specs=vmem(1)[0],
        scratch_shapes=[pltpu.VMEM((2, count, 128), BF16)] * 2,
        compiler_params=params(8),
        cost_estimate=cost(2 * count * 2048 * 512, 8 << 20),
    )(sink_logit, queries, keys_values)
    attn_blocks = kernel_call(
        first_attention_kernel,
        out_shape=tuple([jax.ShapeDtypeStruct((share, 256), BF16)] * NX),
        in_specs=[SMEM] + vmem(4),
        out_specs=tuple(vmem(NX)),
        compiler_params=params(4),
        cost_estimate=cost(1 << 30, 1 << 20),
    )(sink_logit, queries, keys_values, prior, attended)
    attn_blocks = around_x(attn_blocks)

    conv_blocks = kernel_call(
        conv_kernel,
        out_shape=tuple([jax.ShapeDtypeStruct((share + 16, 256), BF16)] * NX),
        in_specs=vmem(5),
        out_specs=tuple(vmem(NX)),
        scratch_shapes=[pltpu.VMEM((8, count + 48, 256), F32), pltpu.VMEM((count, 256), BF16)],
        compiler_params=params(16),
        cost_estimate=cost(2 * count * 2048 * 512, 8 << 20),
    )(glu, prior, conv_weight, conv_bias.reshape(1, -1), channel_gain.reshape(1, -1))
    conv_blocks = around_x(conv_blocks)

    partial_sum = kernel_call(
        functools.partial(out_attn_kernel, tables(attn_parts)),
        out_shape=jax.ShapeDtypeStruct((share, 2048), F32),
        in_specs=vmem(len(attn_parts) + NX),
        out_specs=vmem(1)[0],
        scratch_shapes=[pltpu.VMEM((2048, 1024), BF16), pltpu.VMEM((share, 1024), BF16)],
        compiler_params=params(8),
        cost_estimate=cost(256 * 2048 * 2048, 6 << 20),
    )(*[v for v, _ in attn_parts], *attn_blocks)
    return kernel_call(
        functools.partial(out_conv_kernel, tables(conv_parts)),
        out_shape=jax.ShapeDtypeStruct((share, 2048), BF16),
        in_specs=vmem(len(conv_parts) + NX + 1),
        out_specs=vmem(1)[0],
        scratch_shapes=[pltpu.VMEM((2048, 1024), BF16), pltpu.VMEM((share, 1024), BF16)],
        compiler_params=params(10),
        cost_estimate=cost(256 * 2048 * 2048, 6 << 20),
    )(*[v for v, _ in conv_parts], *conv_blocks, partial_sum)


def solution(mesh):
    torus = Mesh(mesh.devices.reshape(8, 4, 2, mesh.shape["tp"]), ("z", "y", "c", "x"))
    return jax.shard_map(
        shards,
        mesh=torus,
        in_specs=(
            P(SP, None), P(), P(SP, "x"), P(SP, "x"), P(SP, "x"), P(SP, "x"), P(SP, "x"), P("x"),
            P(None, "x"), P("x"), P("x"), P("x", SP), P("x", SP),
        ),
        out_specs=P((*SP, "x"), None),
        check_vma=False,
    )
```
